256 devices in a mesh: sp: 16 (over y, x), tp: 16 (over z, core).
Axes of the slice: x: 4, y: 4, z: 8, core: 2. Of those that a mesh axis runs over, the one named last changes fastest.
Arguments:
- cotangent: bfloat16 [4096, 2048], P('sp', 'tp'), may hold values from -6 to 6
- block_input: bfloat16 [4096, 2048], P('sp', 'tp'), may hold values from -6 to 6
- routes: int32 [4096, 2], P('sp'), may hold values from 0 to 15, all different within a row; in each aligned block of 256 rows (0 to 255, 256 to 511, ...) at most 40 rows name the same one
- route_weights: float32 [4096, 2], P('sp'), may hold values from 0.1 to 0.9
- gate_weight: bfloat16 [16, 2048, 7168], P('sp', None, 'tp'), may hold values from -0.125 to 0.125
- up_weight: bfloat16 [16, 2048, 7168], P('sp', None, 'tp'), may hold values from -0.125 to 0.125
- down_weight: bfloat16 [16, 7168, 2048], P('sp', 'tp'), may hold values from -0.0625 to 0.0625
- out_weight: bfloat16 [1024, 2048], P('tp'), may hold values from -0.1875 to 0.1875
- conv_out: bfloat16 [1024, 4096], P('tp', 'sp'), may hold values from -6 to 6
- gate_pre: bfloat16 [1024, 4096], P('tp', 'sp'), may hold values from -6 to 6
- prior_states: bfloat16 [1024, 4096], P('tp', 'sp'), may hold values from -6 to 6
- recur_weight: bfloat16 [16, 64, 64], replicated, may hold values from -0.75 to 0.75
- input_gate_matrix: bfloat16 [16, 64, 64], replicated, may hold values from -0.75 to 0.75
- decay_param: float32 [1024], replicated, may hold values from 4 to 16
- decay_jump: float32 [1024, 4096], P('tp', 'sp'), may hold values from -1 to 0, as said below
Outputs:
- gate_weight_grad: bfloat16 [16, 2048, 7168], P('sp', None, 'tp')
- up_weight_grad: bfloat16 [16, 2048, 7168], P('sp', None, 'tp')
- down_weight_grad: bfloat16 [16, 7168, 2048], P('sp', 'tp')
- out_weight_grad: float32 [1024, 2048], P('tp', 'sp')
- conv_grad: bfloat16 [1024, 4096], P('tp', 'sp')
- valve_logit_derivative: bfloat16 [1024, 4096], P('tp', 'sp')
The draws below stay inside these ranges and needn't reach their ends.
Inputs may be any that keep to these rules, and one draw needn't show every extreme that they name: In each aligned block of 256 rows (the rows of one index of sp) no expert is named by more than 40 routes, a bound that some block reaches; a row names 2 different experts. `decay_jump`: every entry is at most -1 / 81920.
All inputs are finite; a program needn't handle non-finite values.
Results may differ from the reference program's by a relative error of at most 0.018.
Values may be sent and summed in bfloat16 or wider, within the bound.
No kernel may reach another device: no remote copies, remote signals or barrier semaphores. Data moves between devices by JAX's collectives and lax.ppermute only.
A program may use at most 128 MiB of HBM per device.

```python
import math
import jax
import jax.numpy as jnp
import numpy as np
from jax import lax

D = 2048
HEAD_DIM = 64
HEADS = 16
FF = 7168
TOP_K = 2
TOK_DEV = 256
WIDTH = 1024
EXPERTS = 16
TOKENS = 4096
CAP = 40
N_SP = 16
N_TP = 16


def draw_decay_param(key, part):
    keys = jax.random.split(jax.random.fold_in(key, 11), 3)
    share = 0.5
    fast = jax.random.uniform(keys[0], (WIDTH,), jnp.float32) < share
    fast_rate = jnp.exp(jax.random.uniform(keys[1], (WIDTH,), jnp.float32, jnp.log(1.0 / 400.0), jnp.log(1.0 / 100.0)))
    slow_rate = jnp.exp(jax.random.uniform(keys[2], (WIDTH,), jnp.float32, jnp.log(0.1), jnp.log(0.8))) / (8.0 * TOKENS)
    rate = jnp.where(fast, fast_rate, slow_rate)
    return (-jnp.log(jnp.expm1(rate))).astype(jnp.float32)


def draw_decay_jump(key, part):
    keys = jax.random.split(jax.random.fold_in(key, 23), 3)
    blocks = TOKENS // TOK_DEV
    block_rate = jnp.exp(jax.random.uniform(keys[0], (WIDTH, blocks), jnp.float32, jnp.log(0.05), jnp.log(0.4))) / TOKENS
    settled_regime = jnp.repeat(block_rate, TOK_DEV, axis=1)
    deposit_items = jax.random.randint(keys[1], (2,), 0, TOKENS)
    objective_numbers = jnp.log(jax.random.uniform(keys[2], (WIDTH, 2), jnp.float32, 0.6, 0.8))
    sequence_indices = jnp.arange(TOKENS)[None, :]
    clustered_bundles = jnp.where(sequence_indices == deposit_items[0], objective_numbers[:, 0:1], 0.0) + jnp.where(sequence_indices == deposit_items[1], objective_numbers[:, 1:2], 0.0)
    return (clustered_bundles - settled_regime).astype(jnp.float32)


def spiked(array, stream_key, source, target, blocks, factor):
    def block_of(axis_at):
        return (jnp.arange(array.shape[axis_at]) // (array.shape[axis_at] // blocks)).reshape((-1,) + (1,) * (array.ndim - 1 - axis_at))

    first = jax.random.permutation(stream_key, blocks)[block_of(target)]
    far = (block_of(target) + blocks // 2) % blocks
    return jnp.where((block_of(source) == first) | (block_of(source) == far), factor * array, array)


def steps_of(own_key, dims, cuts, smallest, top_value):
    def one(dim, blocks):
        steps = jax.random.uniform(jax.random.fold_in(jax.random.fold_in(own_key, 6), dim), (blocks,), jnp.float32, smallest / len(cuts), top_value / len(cuts))
        return jnp.repeat(jnp.exp(steps), dims[dim] // blocks).reshape((-1,) + (1,) * (len(dims) - dim - 1))

    factor_of = one(*cuts[0])
    for cut in cuts[1:]:
        factor_of = factor_of * one(*cut)
    return factor_of


def routed_block(own_key, own, number, rows, amount, top, limit, lean):
    order = jax.random.permutation(own_key, amount)
    packed, usual = portions_of(amount, rows * top, limit, lean, True), portions_of(amount, rows * top, limit, lean, False)
    places = jnp.arange(amount)

    def named(lengths, turn):
        used = int((lengths > 0).sum())
        fixed = max(1, used // 4)
        passed = fixed + (places - fixed + turn * (used - fixed)) % max(1, amount - fixed)
        return jnp.zeros((amount,), jnp.int32).at[order[jnp.where(places < fixed, places, passed)]].set(jnp.asarray(lengths, jnp.int32))

    lengths = jnp.where(number % 4 == 0, named(packed, number // 4), named(usual, number - number // 4 - 1))
    mixed = jax.random.permutation(jax.random.fold_in(own, 3), amount)
    donor, taker = mixed[0:amount // 2 * 2:2], mixed[1:amount // 2 * 2:2]
    room = jnp.minimum(lengths[donor] - 1, limit - lengths[taker]) // 2
    room = jnp.where((donor == order[0]) | (taker == order[0]) | (lengths[taker] == 0), 0, jnp.maximum(room, 0))
    passed = jax.random.randint(jax.random.fold_in(own, 4), (amount // 2,), 0, 1 << 20) % (room + 1)
    lengths = lengths.at[donor].add(-passed).at[taker].add(passed)
    items = jnp.searchsorted(jnp.cumsum(lengths), jnp.arange(rows * top), side="right").astype(jnp.int32)
    listing = items.reshape(top, rows).T
    listing = listing[jax.random.permutation(jax.random.fold_in(own, 1), rows)]
    turn = jax.random.randint(jax.random.fold_in(own, 2), (rows, 1), 0, top)
    return jnp.take_along_axis(listing, (jnp.arange(top)[None, :] + turn) % top, axis=1)


def portions_of(amount, total, reach, lean, full):
    loads = [(1 << 20) // math.isqrt(standing ** lean) + 1 for standing in range(1, amount + 1)]
    largest = reach if full else min(reach, max(-(-total // amount), total * loads[0] // sum(loads)))
    least = 1 if total - largest >= amount - 1 else 0
    given, rest = [largest] + [least] * (amount - 1), total - largest - least * (amount - 1)
    while rest > 0:
        free = [i for i in range(1, amount) if given[i] < largest] or [i for i in range(1, amount) if given[i] < reach]
        whole, budget = sum([loads[i] for i in free]), rest
        for i in free:
            extra = min(reach - given[i], max(1, budget * loads[i] // whole), rest)
            given[i] = given[i] + extra
            rest = rest - extra
    return np.array(given)


def noise(own_key, shape, deviation, reach, cuts=(), kind=jnp.bfloat16):
    array = deviation * jax.random.normal(own_key, shape, jnp.float32)
    if cuts:
        array = array * steps_of(own_key, shape, cuts, -0.22, 0.18)
    return jnp.clip(array, -reach, reach).astype(kind)


def heavy_noise(own_key, extent, scale, limit, cuts, heavy, kind=jnp.bfloat16):
    values = scale * jax.random.normal(own_key, extent, jnp.float32)
    if cuts:
        values = values * steps_of(own_key, extent, cuts, -0.22, 0.18)
    return jnp.clip(spiked(values, jax.random.fold_in(own_key, 3), *heavy), -limit, limit).astype(kind)


def setup_inputs(seed: int = 0) -> dict:
    key_of = jax.random.split(jax.random.key(seed), 16)
    cotangent = heavy_noise(key_of[0], (TOKENS, D), 1.0, 6.0, ((0, 16), (1, 16)), (0, 1, 16, 2.0))
    block_input = noise(key_of[1], (TOKENS, D), 1.0, 6.0, ((0, 16), (1, 16)))
    routes_keys = jax.random.split(jax.random.fold_in(key_of[2], 1), TOKENS // TOK_DEV)
    routes_turns = jax.random.permutation(jax.random.fold_in(key_of[2], 3), TOKENS // TOK_DEV)
    routes = jax.vmap(lambda own, number: routed_block(jax.random.fold_in(key_of[2], 2), own, number, TOK_DEV, EXPERTS, TOP_K, CAP, 2))(routes_keys, routes_turns).reshape((TOKENS, TOP_K))
    route_weights = jnp.clip(0.1 + 0.79999997 * jax.random.uniform(key_of[3], (TOKENS, TOP_K), jnp.float32) ** steps_of(key_of[3], (TOKENS, TOP_K), ((0, 16),), -0.2, 0.2), 0.1, 0.9)
    gate_weight = noise(key_of[4], (EXPERTS, D, FF), D ** -0.5, 0.125, ((0, 16), (2, 16)))
    up_weight = noise(key_of[5], (EXPERTS, D, FF), D ** -0.5, 0.125, ((0, 16), (2, 16)))
    down_weight = noise(key_of[6], (EXPERTS, FF, D), FF ** -0.5, 0.0625, ((0, 16), (1, 16)))
    out_weight = noise(key_of[7], (WIDTH, D), WIDTH ** -0.5, 0.1875, ((0, 16),))
    conv_out = noise(key_of[8], (WIDTH, TOKENS), 1.0, 6.0, ((0, 16), (1, 16)))
    gate_pre = noise(key_of[9], (WIDTH, TOKENS), 1.0, 6.0, ((0, 16), (1, 16)))
    prior_states = noise(key_of[10], (WIDTH, TOKENS), 1.0, 6.0, ((0, 16), (1, 16)))
    recur_weight = noise(key_of[11], (HEADS, HEAD_DIM, HEAD_DIM), HEAD_DIM ** -0.5, 0.75)
    input_gate_matrix = noise(key_of[12], (HEADS, HEAD_DIM, HEAD_DIM), HEAD_DIM ** -0.5, 0.75)
    decay_param = draw_decay_param(jax.random.fold_in(key_of[15], 71), 0)
    decay_jump = draw_decay_jump(jax.random.fold_in(key_of[15], 71), 0)
    return dict(cotangent=cotangent, block_input=block_input, routes=routes, route_weights=route_weights, gate_weight=gate_weight, up_weight=up_weight, down_weight=down_weight, out_weight=out_weight, conv_out=conv_out, gate_pre=gate_pre, prior_states=prior_states, recur_weight=recur_weight, input_gate_matrix=input_gate_matrix, decay_param=decay_param, decay_jump=decay_jump)


RATE_SCALE = 8.0

def link_pairs(left_pair, right_pair):
    return (left_pair[0] * right_pair[0], right_pair[0] * left_pair[1] + right_pair[1])

def expert_pass(operands, padded_input, padded_cot):
    index_row, weight_row, w_gate, w_up, w_down = operands
    slot_rows = padded_input[index_row]
    slot_cot = (weight_row[:, None] * padded_cot[index_row].astype(jnp.float32)).astype(jnp.bfloat16)
    gate_act = jnp.dot(slot_rows, w_gate, preferred_element_type=jnp.float32)
    up_act = jnp.dot(slot_rows, w_up, preferred_element_type=jnp.float32)
    sigma_gate = jax.nn.sigmoid(gate_act)
    silu_val = gate_act * sigma_gate
    hidden = (silu_val * up_act).astype(jnp.bfloat16)
    down_grad = jnp.dot(hidden.T, slot_cot, preferred_element_type=jnp.float32).astype(jnp.bfloat16)
    d_hidden = jnp.dot(slot_cot, w_down.T, preferred_element_type=jnp.float32)
    d_gate = (d_hidden * up_act * sigma_gate * (1.0 + gate_act * (1.0 - sigma_gate))).astype(jnp.bfloat16)
    d_up = (d_hidden * silu_val).astype(jnp.bfloat16)
    gate_grad = jnp.dot(slot_rows.T, d_gate, preferred_element_type=jnp.float32).astype(jnp.bfloat16)
    up_grad = jnp.dot(slot_rows.T, d_up, preferred_element_type=jnp.float32).astype(jnp.bfloat16)
    blocks = FF // N_TP
    row_count = index_row.shape[0]
    gate_parts = jnp.einsum('rnf,dnf->nrd', d_gate.astype(jnp.float32).reshape(row_count, N_TP, blocks), w_gate.astype(jnp.float32).reshape(D, N_TP, blocks))
    up_parts = jnp.einsum('rnf,dnf->nrd', d_up.astype(jnp.float32).reshape(row_count, N_TP, blocks), w_up.astype(jnp.float32).reshape(D, N_TP, blocks))
    width_part = lax.optimization_barrier((gate_parts + up_parts).astype(jnp.bfloat16))
    row_grad = lax.optimization_barrier(jnp.sum(width_part.astype(jnp.float32), axis=0)).astype(jnp.bfloat16)
    return (gate_grad, up_grad, down_grad, row_grad)

def reference(cotangent, block_input, routes, route_weights, gate_weight, up_weight, down_weight, out_weight, conv_out, gate_pre, prior_states, recur_weight, input_gate_matrix, decay_param, decay_jump):
    route_count = TOK_DEV * TOP_K
    flat_routes = routes.reshape(N_SP, route_count).astype(jnp.int32)
    onehot = (flat_routes[:, :, None] == jnp.arange(EXPERTS, dtype=jnp.int32)[None, None, :]).astype(jnp.int32)
    slot_rank = lax.optimization_barrier(jnp.sum((jnp.cumsum(onehot, axis=1) - onehot) * onehot, axis=2)).astype(jnp.int32)
    source = jnp.arange(N_SP, dtype=jnp.int32)[:, None]
    position = jnp.arange(route_count, dtype=jnp.int32)[None, :]
    token_ids = (source * TOK_DEV + position // TOP_K).astype(jnp.int32)
    slot_ids = ((flat_routes * N_SP + source) * CAP + slot_rank).astype(jnp.int32)
    total = EXPERTS * N_SP * CAP
    table = jnp.full((total,), TOKENS, jnp.int32).at[slot_ids.reshape(-1)].set(token_ids.reshape(-1))
    weight_table = jnp.zeros((total,), jnp.float32).at[slot_ids.reshape(-1)].set(route_weights.reshape(N_SP, route_count).reshape(-1))
    padded_input = jnp.concatenate([block_input, jnp.zeros((1, D), jnp.bfloat16)], axis=0)
    padded_cot = jnp.concatenate([cotangent, jnp.zeros((1, D), jnp.bfloat16)], axis=0)
    gate_weight_grad, up_weight_grad, down_weight_grad, row_grads = lax.map(partial_expert(padded_input, padded_cot), (table.reshape(EXPERTS, N_SP * CAP), weight_table.reshape(EXPERTS, N_SP * CAP), gate_weight, up_weight, down_weight))
    moe_grad = jnp.zeros((TOKENS + 1, D), jnp.float32).at[table].add(row_grads.reshape(total, D).astype(jnp.float32))[:TOKENS]
    block_grad = (cotangent.astype(jnp.float32) + moe_grad).astype(jnp.bfloat16)
    conv_vals = conv_out.astype(jnp.float32)
    shaped = conv_vals.reshape(HEADS, HEAD_DIM, TOKENS)
    recur_gate = jax.nn.sigmoid(jnp.einsum('hij,hit->hjt', recur_weight.astype(jnp.float32), shaped).reshape(WIDTH, TOKENS))
    input_gate = jax.nn.sigmoid(jnp.einsum('hij,hit->hjt', input_gate_matrix.astype(jnp.float32), shaped).reshape(WIDTH, TOKENS))
    softened = jax.nn.softplus(-decay_param)[:, None]
    log_decay = -RATE_SCALE * recur_gate * softened + decay_jump
    decay_val = jnp.exp(log_decay)
    norm_scale = jnp.sqrt(-jnp.expm1(2.0 * log_decay))
    prior_vals = prior_states.astype(jnp.float32)
    state = decay_val * prior_vals + norm_scale * input_gate * conv_vals
    gate_vals = gate_pre.astype(jnp.float32)
    gelu_val, gelu_pull = jax.vjp(jax.nn.gelu, gate_vals)
    mixed = (gelu_val * state).astype(jnp.bfloat16)
    out_weight_grad = jnp.dot(mixed, block_grad, preferred_element_type=jnp.float32)
    d_mixed = jnp.dot(out_weight, block_grad.T, preferred_element_type=jnp.float32)
    valve_logit_derivative = gelu_pull(d_mixed * state)[0].astype(jnp.bfloat16)
    d_state = d_mixed * gelu_val
    shifted = jnp.concatenate([decay_val[:, 1:], jnp.ones((WIDTH, 1), jnp.float32)], axis=1)
    flipped = lax.associative_scan(link_pairs, (jnp.flip(shifted, 1), jnp.flip(d_state, 1)), axis=1)
    state_grad = jnp.flip(flipped[1], 1)
    grad_log = state_grad * prior_vals * decay_val - state_grad * input_gate * conv_vals * decay_val * decay_val / norm_scale
    grad_recur = (grad_log * -RATE_SCALE * softened * recur_gate * (1.0 - recur_gate)).astype(jnp.bfloat16)
    grad_input = (state_grad * norm_scale * conv_vals * input_gate * (1.0 - input_gate)).astype(jnp.bfloat16)
    back_recur = jnp.einsum('hij,hjt->hit', recur_weight.astype(jnp.float32), grad_recur.astype(jnp.float32).reshape(HEADS, HEAD_DIM, TOKENS)).reshape(WIDTH, TOKENS)
    back_input = jnp.einsum('hij,hjt->hit', input_gate_matrix.astype(jnp.float32), grad_input.astype(jnp.float32).reshape(HEADS, HEAD_DIM, TOKENS)).reshape(WIDTH, TOKENS)
    conv_grad = (state_grad * norm_scale * input_gate + back_recur + back_input).astype(jnp.bfloat16)
    return (gate_weight_grad, up_weight_grad, down_weight_grad, out_weight_grad, conv_grad, valve_logit_derivative)

def partial_expert(padded_input, padded_cot):

    def run_expert(operands):
        return expert_pass(operands, padded_input, padded_cot)
    return run_expert
```

```python
import jax
import jax.numpy as jnp
from jax import lax
from jax.experimental import pallas as pl
from jax.experimental.pallas import tpu as pltpu
from jax.sharding import Mesh
from jax.sharding import PartitionSpec as P

HEAD_DIM = 64
TP = ("z", "c")
CHIPS = 8
SHARDS = 16
CAP = 40
SLOTS = SHARDS * CAP
TOK = 256
COL = 128
RATE_SCALE = 8.0
MIB = 1 << 20


NN = (((1,), (0,)), ((), ()))
NT = (((1,), (1,)), ((), ()))
TN = (((0,), (0,)), ((), ()))
BF = jnp.bfloat16
F32 = jnp.float32


def dot(left, right, dims=NN):
    return lax.dot_general(left, right, dims, preferred_element_type=F32)


def vmem(count):
    return [pl.BlockSpec(memory_space=pltpu.VMEM)] * count


def smem():
    return pl.BlockSpec(memory_space=pltpu.SMEM)


def kernel_call(body, name, outs, scalars, arrays, limit=48):
    return pl.pallas_call(
        body,
        name=name,
        out_shape=outs,
        in_specs=[smem()] * len(scalars) + vmem(len(arrays)),
        out_specs=vmem(len(outs)),
        compiler_params=pltpu.CompilerParams(vmem_limit_bytes=limit * MIB),
    )(*scalars, *arrays)


def out(shape, dtype):
    return jax.ShapeDtypeStruct(shape, dtype)


def spread_body(routes, weights, rows_in, cot_in, sent_rows, sent_cot, placing):
    lanes = lax.broadcasted_iota(jnp.int32, (TOK, COL), 1)
    picks = [routes[:, k : k + 1] for k in range(2)]
    hot = [(pick == lanes).astype(F32) for pick in picks]
    above = lax.broadcasted_iota(jnp.int32, (TOK, TOK), 0)
    left = lax.broadcasted_iota(jnp.int32, (TOK, TOK), 1)
    before = (above > left).astype(F32).astype(BF)
    earlier = dot(before, (hot[0] + hot[1]).astype(BF))
    slots = lax.broadcasted_iota(jnp.int32, (TOK, SLOTS), 1)
    cot = cot_in[...].astype(F32)
    hits = []
    cots = jnp.zeros((SLOTS, COL), F32)
    for k in range(2):
        rank = jnp.sum(earlier * hot[k], axis=1, keepdims=True).astype(jnp.int32)
        hit = (picks[k] * CAP + rank == slots).astype(F32)
        hits.append(hit)
        scaled = (weights[:, k : k + 1] * cot).astype(BF)
        cots = cots + dot(hit.astype(BF), scaled, TN)
    both = (hits[0] + hits[1]).astype(BF)
    placing[...] = both
    sent_rows[...] = dot(both, rows_in[...], TN).astype(BF)
    sent_cot[...] = cots.astype(BF)


def expert_body(place, *refs):
    pieces = refs[:18]
    w_gate, w_up, w_down = refs[18:21]
    rows, cot, hidden, d_gate, d_up, keep, send = refs[21:]
    z = place[0]
    c = place[1]
    for side in range(2):
        core = c if side == 0 else 1 - c
        group = pieces[9 * side : 9 * side + 9]
        shifts = (0, -1, 1, -2, 2, -3, 3)
        for k, shift in enumerate(shifts):
            at = pl.multiple_of((lax.rem(z + shift + CHIPS, CHIPS) * 2 + core) * COL, COL)
            rows[:, pl.ds(at, COL)] = group[k][0]
            cot[:, pl.ds(at, COL)] = group[k][1]
        at = pl.multiple_of((lax.rem(z + 4, CHIPS) * 2 + core) * COL, COL)
        rows[:, pl.ds(at, COL)] = group[7][...]
        cot[:, pl.ds(at, COL)] = group[8][...]
    step = 320
    for m in range(SLOTS // step):
        here = slice(m * step, (m + 1) * step)
        gate = dot(rows[here, :], w_gate[...])
        up = dot(rows[here, :], w_up[...])
        d_hid = dot(cot[here, :], w_down[...], NT)
        sigma = jax.nn.sigmoid(gate)
        silu = gate * sigma
        hidden[here, :] = (silu * up).astype(BF)
        dg = (d_hid * up * sigma * (1.0 + gate * (1.0 - sigma))).astype(BF)
        du = (d_hid * silu).astype(BF)
        d_gate[here, :] = dg
        d_up[here, :] = du
        for target, core in ((send, 1 - c), (keep, c)):
            for p in range(4):
                at = [pl.multiple_of((4 * p + 2 * q + core) * COL, COL) for q in range(2)]
                wg = jnp.concatenate([w_gate[pl.ds(a, COL), :] for a in at], axis=0)
                wu = jnp.concatenate([w_up[pl.ds(a, COL), :] for a in at], axis=0)
                part = dot(dg, wg, NT) + dot(du, wu, NT)
                target[here, 256 * p : 256 * p + 256] = part.astype(BF)


def combine_body(placing, handed, parts):
    total = dot(placing[...], handed[...])
    for k in range(CHIPS):
        parts[k] = total[:, COL * k : COL * k + COL].astype(BF)


def split3(value):
    high = value.astype(BF)
    rest = value - high.astype(F32)
    mid = rest.astype(BF)
    return [part.astype(F32) for part in (high, mid, (rest - mid.astype(F32)).astype(BF))]


def diagonal():
    return lax.broadcasted_iota(jnp.int32, (HEAD_DIM, COL), 0) == lax.broadcasted_iota(
        jnp.int32, (HEAD_DIM, COL), 1
    )


def mixer_body(
    place, own, other, out_weight, mixed, gelu_val, gelu_state, decay, valve, payload, local, passed
):
    c = place[1]
    total = jnp.zeros((HEAD_DIM, TOK), F32)
    mix = mixed[...]
    for ref, core in ((own, c), (other, 1 - c)):
        for k in range(CHIPS):
            at = 2 * k + core
            block = ref[k]
            cols = out_weight[:, pl.ds(pl.multiple_of(at * COL, COL), COL)]
            total = total + dot(cols, block, NT)
            payload[at, 0:HEAD_DIM, :] = dot(mix, block).astype(BF)
    valve[...] = (total * gelu_state[...]).astype(BF)
    lanes = lax.broadcasted_iota(jnp.int32, (HEAD_DIM, TOK), 1)
    first = decay[:, 0:1]
    coef = jnp.where(lanes < TOK - 1, pltpu.roll(decay[...], TOK - 1, 1), 1.0)
    value = total * gelu_val[...]
    reach = 1
    while reach < TOK:
        inside = lanes < TOK - reach
        value = value + coef * jnp.where(inside, pltpu.roll(value, TOK - reach, 1), 0.0)
        coef = coef * jnp.where(inside, pltpu.roll(coef, TOK - reach, 1), 1.0)
        reach *= 2
    local[...] = value
    passed[...] = coef
    eye = diagonal()
    lines = []
    for column in (first * coef[:, 0:1], first * value[:, 0:1]):
        line = jnp.sum(jnp.where(eye, column, 0.0), axis=0, keepdims=True)
        lines += split3(line)
    block = jnp.concatenate(lines + [jnp.zeros((10, COL), F32)], axis=0).astype(BF)
    for k in range(SHARDS):
        payload[k, HEAD_DIM:80, :] = block


def finish_body(
    place, got, local, passed, on_recur, on_input, direct, w_recur, w_input, out_grad, conv_grad
):
    s = place[2]
    total = got[0, 0:HEAD_DIM, :].astype(F32)
    for k in range(1, SHARDS):
        total = total + got[k, 0:HEAD_DIM, :].astype(F32)
    out_grad[...] = total
    carry = jnp.zeros((1, COL), F32)
    for k in range(SHARDS - 1, 0, -1):
        lines = got[k, HEAD_DIM:80, :].astype(F32)
        factor = lines[0:1] + lines[1:2] + lines[2:3]
        added = lines[3:4] + lines[4:5] + lines[5:6]
        carry = jnp.where(k > s, added + factor * carry, carry)
    column = jnp.sum(jnp.where(diagonal(), carry, 0.0), axis=1, keepdims=True)
    grad = local[...] + passed[...] * column
    by_recur = (grad * on_recur[...]).astype(BF)
    by_input = (grad * on_input[...]).astype(BF)
    conv_grad[...] = (
        grad * direct[...] + dot(w_recur[...], by_recur) + dot(w_input[...], by_input)
    ).astype(BF)


def ring(step):
    return [(k, (k + step) % CHIPS) for k in range(CHIPS)]


def swap(value):
    return lax.ppermute(value, "c", [(0, 1), (1, 0)])


def gathered(value):
    pieces = [value]
    ahead = behind = value
    for _ in range(3):
        ahead = lax.ppermute(ahead, "z", ring(1))
        behind = lax.ppermute(behind, "z", ring(-1))
        pieces += [ahead, behind]
    pieces.append(lax.ppermute(ahead[0], "z", ring(1)))
    pieces.append(lax.ppermute(behind[1], "z", ring(-1)))
    return pieces + [swap(piece) for piece in pieces]


def local(
    cotangent,
    block_input,
    routes,
    route_weights,
    gate_weight,
    up_weight,
    down_weight,
    out_weight,
    conv_out,
    gate_pre,
    prior_states,
    recur_weight,
    input_gate_matrix,
    decay_param,
    decay_jump,
):
    z = lax.axis_index("z")
    c = lax.axis_index("c")
    place = jnp.stack([z, c, lax.axis_index("sp")]).astype(jnp.int32)
    sent_rows, sent_cot, placing = kernel_call(
        spread_body,
        "spread",
        (out((SLOTS, COL), BF), out((SLOTS, COL), BF), out((TOK, SLOTS), BF)),
        (),
        (routes, route_weights, block_input, cotangent),
    )
    sent = jnp.concatenate(
        [sent_rows.reshape(SHARDS, CAP, COL), sent_cot.reshape(SHARDS, CAP, COL)], axis=1
    )
    got = lax.all_to_all(sent, "sp", 0, 0, tiled=True)
    pair = jnp.stack([got[:, :CAP].reshape(SLOTS, COL), got[:, CAP:].reshape(SLOTS, COL)])
    pieces = gathered(pair)
    width = gate_weight.shape[2]
    model = gate_weight.shape[1]
    rows, cot, hidden, d_gate, d_up, keep, send = kernel_call(
        expert_body,
        "expert",
        (
            out((SLOTS, model), BF),
            out((SLOTS, model), BF),
            out((SLOTS, width), BF),
            out((SLOTS, width), BF),
            out((SLOTS, width), BF),
            out((SLOTS, model // 2), BF),
            out((SLOTS, model // 2), BF),
        ),
        (place,),
        (*pieces, gate_weight[0], up_weight[0], down_weight[0]),
        60,
    )
    arrived = swap(send)
    summed = (keep.astype(F32) + arrived.astype(F32)).astype(BF)
    handed = lax.all_to_all(
        summed.reshape(SHARDS, CAP, model // 2), "sp", 0, 0, tiled=True
    ).reshape(SLOTS, model // 2)
    gate_grad = dot(rows, d_gate, TN).astype(BF)
    up_grad = dot(rows, d_up, TN).astype(BF)
    down_grad = dot(hidden, cot, TN).astype(BF)
    (parts,) = kernel_call(
        combine_body, "combine", (out((CHIPS, TOK, COL), BF),), (), (placing, handed)
    )
    parts = lax.all_to_all(parts, "z", 0, 0, tiled=True)
    block_grad = (cotangent.astype(F32) + jnp.sum(parts.astype(F32), axis=0)).astype(BF)
    own = lax.all_to_all(
        jnp.broadcast_to(block_grad[None], (CHIPS, TOK, COL)), "z", 0, 0, tiled=True
    )
    other = swap(own)

    head = 2 * z + c
    w_recur = lax.dynamic_index_in_dim(recur_weight, head, 0, keepdims=False)
    w_input = lax.dynamic_index_in_dim(input_gate_matrix, head, 0, keepdims=False)
    softened = jax.nn.softplus(
        -lax.dynamic_slice_in_dim(decay_param, head * HEAD_DIM, HEAD_DIM, 0)
    )[:, None]
    recur_gate = jax.nn.sigmoid(dot(w_recur, conv_out, TN))
    input_gate = jax.nn.sigmoid(dot(w_input, conv_out, TN))
    log_decay = -RATE_SCALE * recur_gate * softened + decay_jump
    decay_val = jnp.exp(log_decay)
    norm_scale = jnp.sqrt(-jnp.expm1(2.0 * log_decay))
    conv_vals = conv_out.astype(F32)
    prior_vals = prior_states.astype(F32)
    state = decay_val * prior_vals + norm_scale * input_gate * conv_vals
    gelu_val, gelu_pull = jax.vjp(jax.nn.gelu, gate_pre.astype(F32))
    mixed = (gelu_val * state).astype(BF)
    gelu_state = gelu_pull(state)[0]
    on_log = prior_vals * decay_val - input_gate * conv_vals * decay_val * decay_val / norm_scale
    on_recur = on_log * -RATE_SCALE * softened * recur_gate * (1.0 - recur_gate)
    on_input = norm_scale * conv_vals * input_gate * (1.0 - input_gate)
    direct = norm_scale * input_gate

    valve, payload, local_sum, passed = kernel_call(
        mixer_body,
        "mixer",
        (
            out((HEAD_DIM, TOK), BF),
            out((SHARDS, 80, COL), BF),
            out((HEAD_DIM, TOK), F32),
            out((HEAD_DIM, TOK), F32),
        ),
        (place,),
        (own, other, out_weight, mixed, gelu_val, gelu_state, decay_val),
    )
    replies = lax.all_to_all(payload, "sp", 0, 0, tiled=True)
    out_grad, conv_grad = kernel_call(
        finish_body,
        "finish",
        (out((HEAD_DIM, COL), F32), out((HEAD_DIM, TOK), BF)),
        (place,),
        (replies, local_sum, passed, on_recur, on_input, direct, w_recur, w_input),
    )
    return (gate_grad[None], up_grad[None], down_grad[None], out_grad, conv_grad, valve)


def solution(mesh):
    split = Mesh(mesh.devices.reshape(mesh.shape["sp"], CHIPS, 2), ("sp", "z", "c"))
    return jax.shard_map(
        local,
        mesh=split,
        in_specs=(
            P("sp", TP),
            P("sp", TP),
            P("sp", None),
            P("sp", None),
            P("sp", None, TP),
            P("sp", None, TP),
            P("sp", TP, None),
            P(TP, None),
            P(TP, "sp"),
            P(TP, "sp"),
            P(TP, "sp"),
            P(),
            P(),
            P(),
            P(TP, "sp"),
        ),
        out_specs=(
            P("sp", None, TP),
            P("sp", None, TP),
            P("sp", TP, None),
            P(TP, "sp"),
            P(TP, "sp"),
            P(TP, "sp"),
        ),
        check_vma=False,
    )
```

```python
import jax
import jax.numpy as jnp
from jax import lax
from jax.experimental import pallas as pl
from jax.experimental.pallas import tpu as pltpu
from jax.sharding import Mesh
from jax.sharding import PartitionSpec as P

HEAD_DIM = 64
TP = ("z", "c")
CHIPS = 8
SHARDS = 16
CAP = 40
SLOTS = SHARDS * CAP
TOK = 256
COL = 128
RATE_SCALE = 8.0
MIB = 1 << 20


NN = (((1,), (0,)), ((), ()))
NT = (((1,), (1,)), ((), ()))
TN = (((0,), (0,)), ((), ()))
BF = jnp.bfloat16
F32 = jnp.float32


def dot(left, right, dims=NN):
    return lax.dot_general(left, right, dims, preferred_element_type=F32)


def spec(kind):
    return pl.BlockSpec(memory_space={"v": pltpu.VMEM, "h": pltpu.HBM, "s": pltpu.SMEM}[kind])


def kernel_call(body, name, outs, arrays, kinds, out_kinds, scratch=(), limit=16, aliases=None):
    return pl.pallas_call(
        body,
        name=name,
        out_shape=outs,
        in_specs=[spec(kind) for kind in kinds],
        out_specs=tuple(spec(kind) for kind in out_kinds),
        scratch_shapes=list(scratch),
        input_output_aliases=aliases or {},
        compiler_params=pltpu.CompilerParams(vmem_limit_bytes=limit * MIB),
    )(*arrays)


class Copies:
    def __init__(self, sems):
        self.sems = sems
        self.used = 0

    def start(self, source, target):
        copy = pltpu.make_async_copy(source, target, self.sems.at[self.used])
        self.used += 1
        copy.start()
        return copy


def wait_all(copies):
    for copy in copies:
        copy.wait()


def sems(count):
    return pltpu.SemaphoreType.DMA((count,))


def out(shape, dtype):
    return jax.ShapeDtypeStruct(shape, dtype)


def spread_body(
    routes_h, weights_h, rows_h, cot_h, sent, placing, routes, weights, rows_in, cot_in, sem
):
    copies = Copies(sem)
    wait_all(
        [
            copies.start(*pair)
            for pair in (
                (routes_h, routes),
                (weights_h, weights),
                (rows_h, rows_in),
                (cot_h, cot_in),
            )
        ]
    )
    lanes = lax.broadcasted_iota(jnp.int32, (TOK, COL), 1)
    lines = jnp.concatenate(
        [routes[...].astype(F32), weights[...], jnp.zeros((4, TOK), F32)], axis=0
    )
    columns = lines.T
    picks = [columns[:, k : k + 1].astype(jnp.int32) for k in range(2)]
    hot = [(pick == lanes).astype(F32) for pick in picks]
    above = lax.broadcasted_iota(jnp.int32, (TOK, TOK), 0)
    left = lax.broadcasted_iota(jnp.int32, (TOK, TOK), 1)
    before = (above > left).astype(F32).astype(BF)
    earlier = dot(before, (hot[0] + hot[1]).astype(BF))
    slots = lax.broadcasted_iota(jnp.int32, (TOK, SLOTS), 1)
    cot = cot_in[...].astype(F32)
    hits = []
    cots = jnp.zeros((SLOTS, COL), F32)
    for k in range(2):
        rank = jnp.sum(earlier * hot[k], axis=1, keepdims=True).astype(jnp.int32)
        hit = (picks[k] * CAP + rank == slots).astype(F32)
        hits.append(hit)
        scaled = (columns[:, k + 2 : k + 3] * cot).astype(BF)
        cots = cots + dot(hit.astype(BF), scaled, TN)
    both = (hits[0] + hits[1]).astype(BF)
    placing[...] = both
    rows = dot(both, rows_in[...], TN)
    sent[...] = jnp.concatenate(
        [rows.reshape(SHARDS, CAP, COL), cots.reshape(SHARDS, CAP, COL)], axis=1
    ).astype(BF)


def parity_columns(weight, pair, core):
    at = [pl.multiple_of((4 * pair + 2 * k + core) * COL, COL) for k in range(2)]
    return jnp.concatenate([weight[:, pl.ds(a, COL)] for a in at], axis=1)


def expert_body(*refs):
    pieces = refs[:16]
    gate_h, up_h, down_h = refs[16:19]
    rows_out, cot_out, hidden_out, gate_out, up_out, send_out, keep_out = refs[19:26]
    rows, cot, w_gate, w_up, w_down, hidden, d_gate, d_up, send, keep, sem = refs[26:]
    z = lax.axis_index("z")
    c = lax.axis_index("c")
    copies = Copies(sem)
    step = SLOTS // 2
    width = w_gate.shape[0]
    halves = [slice(m * step, (m + 1) * step) for m in range(2)]
    spots = []
    for side in range(2):
        core = c if side == 0 else 1 - c
        for k, shift in enumerate((0, -1, 1, -2, 2, -3, 3, -4)):
            at = pl.multiple_of((lax.rem(z + shift + CHIPS, CHIPS) * 2 + core) * COL, COL)
            spots.append((pieces[CHIPS * side + k], at))

    def load(kind, target, here):
        return [
            copies.start(piece.at[kind, here, :], target.at[here, pl.ds(at, COL)])
            for piece, at in spots
        ]

    for_gate = [load(0, rows, halves[0]) + [copies.start(gate_h, w_gate)]]
    for_up = [copies.start(up_h, w_up)]
    for_down = [load(1, cot, halves[0]) + [copies.start(down_h, w_down)]]
    for_gate.append(load(0, rows, halves[1]))
    for_down.append(load(1, cot, halves[1]))
    stored = []
    for m in range(2):
        here = halves[m]
        wait_all(for_gate[m])
        stored.append(copies.start(rows.at[here, :], rows_out.at[here, :]))
        gate = dot(rows[here, :], w_gate[...], NT)
        if m == 0:
            wait_all(for_up)
        up = dot(rows[here, :], w_up[...], NT)
        wait_all(for_down[m])
        stored.append(copies.start(cot.at[here, :], cot_out.at[here, :]))
        d_hid = dot(cot[here, :], w_down[...], NT)
        sigma = jax.nn.sigmoid(gate)
        silu = gate * sigma
        hidden[here, :width] = (silu * up).astype(BF)
        dg = (d_hid * up * sigma * (1.0 + gate * (1.0 - sigma))).astype(BF)
        du = (d_hid * silu).astype(BF)
        d_gate[here, :width] = dg
        d_up[here, :width] = du
        for near in (hidden, d_gate, d_up):
            near[here, width:] = jnp.zeros((step, near.shape[1] - width), BF)
        for near, far in ((hidden, hidden_out), (d_gate, gate_out), (d_up, up_out)):
            stored.append(copies.start(near.at[here, :], far.at[here, :]))
        for core, near, far in ((1 - c, send, send_out), (c, keep, keep_out)):
            for p in range(4):
                part = dot(dg, parity_columns(w_gate, p, core)) + dot(
                    du, parity_columns(w_up, p, core)
                )
                near[here, 256 * p : 256 * p + 256] = part.astype(BF)
            stored.append(copies.start(near.at[here, :], far.at[here, :]))
    wait_all(stored)


def combine_body(placing, handed, _, parts):
    total = dot(placing[...], handed[...])
    for k in range(CHIPS):
        parts[k] = total[:, COL * k : COL * k + COL].astype(BF)


def split3(value):
    high = value.astype(BF)
    rest = value - high.astype(F32)
    mid = rest.astype(BF)
    return [part.astype(F32) for part in (high, mid, (rest - mid.astype(F32)).astype(BF))]


def diagonal():
    return lax.broadcasted_iota(jnp.int32, (HEAD_DIM, COL), 0) == lax.broadcasted_iota(
        jnp.int32, (HEAD_DIM, COL), 1
    )


def half_body(own, out_weight, mixed, begun, payload):
    c = lax.axis_index("c")
    total = jnp.zeros((HEAD_DIM, TOK), F32)
    mix = mixed[...]
    for k in range(CHIPS):
        block = own[k]
        cols = out_weight[:, pl.ds(pl.multiple_of((2 * k + c) * COL, COL), COL)]
        total = total + dot(cols, block, NT)
        payload[k] = dot(mix, block).astype(BF)
    begun[...] = total


def mixer_body(
    other, out_weight, mixed, begun, first_half, gelu_val, gelu_state, decay, valve, payload, local, passed
):
    c = lax.axis_index("c")
    total = begun[...]
    mix = mixed[...]
    for k in range(CHIPS):
        at = 2 * k + 1 - c
        block = other[k]
        cols = out_weight[:, pl.ds(pl.multiple_of(at * COL, COL), COL)]
        total = total + dot(cols, block, NT)
        payload[at, 0:HEAD_DIM, :] = dot(mix, block).astype(BF)
        payload[2 * k + c, 0:HEAD_DIM, :] = first_half[k]
    valve[...] = (total * gelu_state[...]).astype(BF)
    lanes = lax.broadcasted_iota(jnp.int32, (HEAD_DIM, TOK), 1)
    first = decay[:, 0:1]
    coef = jnp.where(lanes < TOK - 1, pltpu.roll(decay[...], TOK - 1, 1), 1.0)
    value = total * gelu_val[...]
    reach = 1
    while reach < TOK:
        inside = lanes < TOK - reach
        value = value + coef * jnp.where(inside, pltpu.roll(value, TOK - reach, 1), 0.0)
        coef = coef * jnp.where(inside, pltpu.roll(coef, TOK - reach, 1), 1.0)
        reach *= 2
    local[...] = value
    passed[...] = coef
    eye = diagonal()
    lines = []
    for column in (first * coef[:, 0:1], first * value[:, 0:1]):
        line = jnp.sum(jnp.where(eye, column, 0.0), axis=0, keepdims=True)
        lines += split3(line)
    block = jnp.concatenate(lines + [jnp.zeros((10, COL), F32)], axis=0).astype(BF)
    for k in range(SHARDS):
        payload[k, HEAD_DIM:80, :] = block


def finish_body(
    got, local, passed, on_recur, on_input, direct, w_recur, w_input, out_grad, conv_grad
):
    s = lax.axis_index("sp")
    total = got[0, 0:HEAD_DIM, :].astype(F32)
    for k in range(1, SHARDS):
        total = total + got[k, 0:HEAD_DIM, :].astype(F32)
    out_grad[...] = total
    carry = jnp.zeros((1, COL), F32)
    for k in range(SHARDS - 1, 0, -1):
        lines = got[k, HEAD_DIM:80, :].astype(F32)
        factor = lines[0:1] + lines[1:2] + lines[2:3]
        added = lines[3:4] + lines[4:5] + lines[5:6]
        carry = jnp.where(k > s, added + factor * carry, carry)
    column = jnp.sum(jnp.where(diagonal(), carry, 0.0), axis=1, keepdims=True)
    grad = local[...] + passed[...] * column
    by_recur = (grad * on_recur[...]).astype(BF)
    by_input = (grad * on_input[...]).astype(BF)
    conv_grad[...] = (
        grad * direct[...] + dot(w_recur[...], by_recur) + dot(w_input[...], by_input)
    ).astype(BF)


def ring(step):
    return [(k, (k + step) % CHIPS) for k in range(CHIPS)]


def swap(value):
    return lax.ppermute(value, "c", [(0, 1), (1, 0)])


def gathered(values):
    ahead = behind = jnp.stack(values)
    pieces = [ahead]
    for _ in range(3):
        ahead = lax.ppermute(ahead, "z", ring(1))
        behind = lax.ppermute(behind, "z", ring(-1))
        pieces += [ahead, behind]
    pieces.append(lax.ppermute(ahead, "z", ring(1)))
    return pieces + [swap(piece) for piece in pieces]


def local(
    cotangent,
    block_input,
    routes,
    route_weights,
    gate_weight,
    up_weight,
    down_weight,
    out_weight,
    conv_out,
    gate_pre,
    prior_states,
    recur_weight,
    input_gate_matrix,
    decay_param,
    decay_jump,
):
    z = lax.axis_index("z")
    c = lax.axis_index("c")
    sent, placing = kernel_call(
        spread_body,
        "spread",
        (out((SHARDS, 2 * CAP, COL), BF), out((TOK, SLOTS), BF)),
        (routes.T, route_weights.T, block_input, cotangent),
        "hhhh",
        "vv",
        (
            pltpu.VMEM((2, TOK), jnp.int32),
            pltpu.VMEM((2, TOK), F32),
            pltpu.VMEM((TOK, COL), BF),
            pltpu.VMEM((TOK, COL), BF),
            sems(4),
        ),
        60,
    )
    got = lax.all_to_all(sent, "sp", 0, 0, tiled=True)
    pieces = gathered([got[:, :CAP].reshape(SLOTS, COL), got[:, CAP:].reshape(SLOTS, COL)])
    width = gate_weight.shape[2]
    model = gate_weight.shape[1]
    weights = (gate_weight[0].T, up_weight[0].T, down_weight[0])
    wide = (SLOTS, model)
    thin = (SLOTS, -(-width // COL) * COL)
    half = (SLOTS, model // 2)
    shapes = [wide, wide, thin, thin, thin, half, half]
    rows, cot, hidden, d_gate, d_up, send, keep = kernel_call(
        expert_body,
        "expert",
        tuple(out(shape, BF) for shape in shapes),
        (*pieces, *weights),
        "h" * 19,
        "h" * 7,
        [pltpu.VMEM(wide, BF)] * 2
        + [pltpu.VMEM((width, model), BF)] * 3
        + [pltpu.VMEM(shape, BF) for shape in shapes[2:]]
        + [sems(90)],
        60,
    )
    arrived = swap(send)
    gate_grad = dot(d_gate[:, :width], rows, TN).astype(BF)
    summed = (keep.astype(F32) + arrived.astype(F32)).astype(BF)
    handed = lax.all_to_all(
        summed.reshape(SHARDS, CAP, model // 2), "sp", 0, 0, tiled=True
    ).reshape(SLOTS, model // 2)
    up_grad = dot(d_up[:, :width], rows, TN).astype(BF)
    down_grad = dot(hidden[:, :width], cot, TN).astype(BF)
    grads = (gate_grad, up_grad, down_grad)
    done = sum(grad[:8, :COL].astype(F32) for grad in grads)
    (parts,) = kernel_call(
        combine_body,
        "combine",
        (out((CHIPS, TOK, COL), BF),),
        (placing, handed, done),
        "vvv",
        "v",
    )
    parts = lax.all_to_all(parts, "z", 0, 0, tiled=True)
    block_grad = (cotangent.astype(F32) + jnp.sum(parts.astype(F32), axis=0)).astype(BF)
    own = lax.all_to_all(
        jnp.broadcast_to(block_grad[None], (CHIPS, TOK, COL)), "z", 0, 0, tiled=True
    )
    other = swap(own)

    head = 2 * z + c
    w_recur = lax.dynamic_index_in_dim(recur_weight, head, 0, keepdims=False)
    w_input = lax.dynamic_index_in_dim(input_gate_matrix, head, 0, keepdims=False)
    softened = jax.nn.softplus(
        -lax.dynamic_slice_in_dim(decay_param, head * HEAD_DIM, HEAD_DIM, 0)
    )[:, None]
    recur_gate = jax.nn.sigmoid(dot(w_recur, conv_out, TN))
    input_gate = jax.nn.sigmoid(dot(w_input, conv_out, TN))
    log_decay = -RATE_SCALE * recur_gate * softened + decay_jump
    decay_val = jnp.exp(log_decay)
    norm_scale = jnp.sqrt(-jnp.expm1(2.0 * log_decay))
    conv_vals = conv_out.astype(F32)
    prior_vals = prior_states.astype(F32)
    state = decay_val * prior_vals + norm_scale * input_gate * conv_vals
    gelu_val, gelu_pull = jax.vjp(jax.nn.gelu, gate_pre.astype(F32))
    mixed = (gelu_val * state).astype(BF)
    gelu_state = gelu_pull(state)[0]
    on_log = prior_vals * decay_val - input_gate * conv_vals * decay_val * decay_val / norm_scale
    on_recur = on_log * -RATE_SCALE * softened * recur_gate * (1.0 - recur_gate)
    on_input = norm_scale * conv_vals * input_gate * (1.0 - input_gate)
    direct = norm_scale * input_gate

    begun, first_half = kernel_call(
        half_body,
        "half",
        (out((HEAD_DIM, TOK), F32), out((CHIPS, HEAD_DIM, COL), BF)),
        (own, out_weight, mixed),
        "vvv",
        "vv",
    )
    valve, payload, local_sum, passed = kernel_call(
        mixer_body,
        "mixer",
        (
            out((HEAD_DIM, TOK), BF),
            out((SHARDS, 80, COL), BF),
            out((HEAD_DIM, TOK), F32),
            out((HEAD_DIM, TOK), F32),
        ),
        (other, out_weight, mixed, begun, first_half, gelu_val, gelu_state, decay_val),
        "vvvvvvvv",
        "vvvv",
    )
    replies = lax.all_to_all(payload, "sp", 0, 0, tiled=True)
    out_grad, conv_grad = kernel_call(
        finish_body,
        "finish",
        (out((HEAD_DIM, COL), F32), out((HEAD_DIM, TOK), BF)),
        (replies, local_sum, passed, on_recur, on_input, direct, w_recur, w_input),
        "vvvvvvvv",
        "vv",
    )
    return (gate_grad.T[None], up_grad.T[None], down_grad[None], out_grad, conv_grad, valve)


def solution(mesh):
    split = Mesh(mesh.devices.reshape(mesh.shape["sp"], CHIPS, 2), ("sp", "z", "c"))
    return jax.shard_map(
        local,
        mesh=split,
        in_specs=(
            P("sp", TP),
            P("sp", TP),
            P("sp", None),
            P("sp", None),
            P("sp", None, TP),
            P("sp", None, TP),
            P("sp", TP, None),
            P(TP, None),
            P(TP, "sp"),
            P(TP, "sp"),
            P(TP, "sp"),
            P(),
            P(),
            P(),
            P(TP, "sp"),
        ),
        out_specs=(
            P("sp", None, TP),
            P("sp", None, TP),
            P("sp", TP, None),
            P(TP, "sp"),
            P(TP, "sp"),
            P(TP, "sp"),
        ),
        check_vma=False,
    )
```
